256 devices in a mesh: grp: 2 (over y), sp: 32 (over z, core), tp: 4 (over x).
Axes of the slice: x: 4, y: 2, z: 16, core: 2. Of those that a mesh axis runs over, the one named last changes fastest.
The devices are a block of a 4x16x16 slice.
Arguments:
- conv_input: bfloat16 [32768, 1024], P(('grp', 'sp'), 'tp'), parts along dimension 0, may hold values from -6 to 6
- pre_gate: bfloat16 [32768, 1024], P(('grp', 'sp'), 'tp'), parts along dimension 0, may hold values from -6 to 6
- post_gate: bfloat16 [32768, 1024], P(('grp', 'sp'), 'tp'), parts along dimension 0, may hold values from -6 to 6
- conv_taps: float32 [3, 1024], replicated, may hold values from -3.5 to 3.5
- out_proj: bfloat16 [1024, 2048], replicated, may hold values from -0.1875 to 0.1875
- residual_in: bfloat16 [32768, 2048], P(('grp', 'sp', 'tp')), parts along dimension 0, may hold values from -6 to 6
- norm_gain: float32 [2048], replicated, may hold values from 0.1 to 1.9
- routes: int32 [32768, 2], P(('grp', 'sp', 'tp')), parts along dimension 0, may hold values from 0 to 63, as said below
- route_weight: float32 [32768, 2], P(('grp', 'sp', 'tp')), parts along dimension 0, may hold values from 0.1 to 1
- w_gate: bfloat16 [64, 2048, 1024], P('sp', None, 'tp'), may hold values from -0.125 to 0.125
- w_up: bfloat16 [64, 2048, 1024], P('sp', None, 'tp'), may hold values from -0.125 to 0.125
- w_down: bfloat16 [64, 1024, 2048], P('sp', 'tp'), may hold values from -0.1875 to 0.1875
Outputs:
- layer_out: bfloat16 [32768, 2048], P(('grp', 'sp', 'tp')), parts along dimension 0
The draws below stay inside these ranges and needn't reach their ends.
There are 2 independent parts, one for each index of `grp`. The reference program is written for one: setup_inputs(seed, part) draws one part's arguments, and reference() takes and returns one part's arrays. A program takes and returns all parts, laid end to end along the dimension named above; an argument that names none is the same for every part. Nothing has to cross between parts.
Inputs may be any that keep to these rules, and one draw needn't show every extreme that they name: `routes`: the two numbers of a row differ and lie in the same group of 16 consecutive experts. In each aligned block of 128 rows every expert is named exactly 4 times.
All inputs are finite; a program needn't handle non-finite values.
Results may differ from the reference program's by a relative error of at most 0.0085.
Values may be sent and summed in bfloat16 or wider, within the bound.
A program may use at most 64 MiB of HBM per device.

```python
import jax
import jax.numpy as jnp
from jax import lax

D = 2048
CH = 1024
HID = 1024
CONV = 3
GROUPS = 4
TOKENS = 16384
EXPERTS = 64
EPG = 16
ROW_BLOCK = 128
BLOCKS = 128
N_TP = 4


def draw_routes(key, part):
    base = jax.random.fold_in(key, 7)
    perm_key, shift_key = jax.random.split(base)
    block_keys = jax.random.split(perm_key, BLOCKS)
    ranks = jax.vmap(lambda k: jax.random.permutation(k, ROW_BLOCK))(block_keys).astype(jnp.int32)
    offsets = jax.random.randint(shift_key, (BLOCKS, 1), 0, EPG // 2).astype(jnp.int32)
    group = ranks % GROUPS
    within = ranks // GROUPS
    first = 2 * within % EPG
    second = (2 * within + 1 + 2 * offsets) % EPG
    chosen = jnp.stack([group * EPG + first, group * EPG + second], axis=-1)
    return chosen.reshape(TOKENS, 2).astype(jnp.int32)


def block_scale(own_key, shape, cuts, least, high):
    level = 1.0
    for position, shards_of in cuts:
        steps = jax.random.uniform(jax.random.fold_in(jax.random.fold_in(own_key, 6), position), (shards_of,), jnp.float32, least / len(cuts), high / len(cuts))
        level = level * jnp.repeat(jnp.exp(steps), shape[position] // shards_of).reshape((-1,) + (1,) * (len(shape) - 1 - position))
    return level


def gaussian(rng, dims, spread, most, pieces=(), held_as=jnp.bfloat16):
    entries = spread * jax.random.normal(rng, dims, jnp.float32)
    if pieces:
        entries = entries * block_scale(rng, dims, pieces, -0.22, 0.18)
    return jnp.clip(entries, -most, most).astype(held_as)


def setup_inputs(seed: int = 0, part: int = 0) -> dict:
    key_of = jax.random.split(jax.random.key(seed), 13)
    part_splits = jax.random.split(jax.random.fold_in(key_of[12], part), 13)
    conv_input = gaussian(part_splits[0], (TOKENS, CH), 1.0, 6.0, ((0, 32), (1, 4)))
    pre_gate = gaussian(part_splits[1], (TOKENS, CH), 1.0, 6.0, ((0, 32), (1, 4)))
    post_gate = gaussian(part_splits[2], (TOKENS, CH), 1.0, 6.0, ((0, 32), (1, 4)))
    conv_taps = gaussian(key_of[3], (CONV, CH), CONV ** -0.5, 3.5, (), jnp.float32)
    out_proj = gaussian(key_of[4], (CH, D), CH ** -0.5, 0.1875)
    residual_in = gaussian(part_splits[5], (TOKENS, D), 1.0, 6.0, ((0, 128),))
    norm_gain = jnp.clip(1.0 + 0.18 * jax.random.normal(key_of[6], (D,), jnp.float32), 0.1, 1.9)
    routes = draw_routes(jax.random.fold_in(jax.random.fold_in(key_of[12], part), 71), part)
    route_weight = jnp.clip(0.1 + 0.9 * jax.random.uniform(part_splits[8], (TOKENS, 2), jnp.float32) ** block_scale(part_splits[8], (TOKENS, 2), ((0, 128),), -0.2, 0.2), 0.1, 1.0)
    w_gate = gaussian(key_of[9], (EXPERTS, D, HID), D ** -0.5, 0.125, ((0, 32), (2, 4)))
    w_up = gaussian(key_of[10], (EXPERTS, D, HID), D ** -0.5, 0.125, ((0, 32), (2, 4)))
    w_down = gaussian(key_of[11], (EXPERTS, HID, D), HID ** -0.5, 0.1875, ((0, 32), (1, 4)))
    return dict(conv_input=conv_input, pre_gate=pre_gate, post_gate=post_gate, conv_taps=conv_taps, out_proj=out_proj, residual_in=residual_in, norm_gain=norm_gain, routes=routes, route_weight=route_weight, w_gate=w_gate, w_up=w_up, w_down=w_down)


def reference(conv_input, pre_gate, post_gate, conv_taps, out_proj, residual_in, norm_gain, routes, route_weight, w_gate, w_up, w_down):
    gated = pre_gate.astype(jnp.float32) * conv_input.astype(jnp.float32)
    padded = jnp.pad(gated, ((2, 0), (0, 0)))
    conv = padded[2:] * conv_taps[2] + padded[1:-1] * conv_taps[1] + padded[:-2] * conv_taps[0]
    mixed = (post_gate.astype(jnp.float32) * conv).astype(jnp.bfloat16)
    projected = jnp.dot(mixed, out_proj, preferred_element_type=jnp.float32)
    stream = residual_in.astype(jnp.float32) + projected
    scale = lax.rsqrt(lax.optimization_barrier(jnp.mean(stream * stream, axis=-1, keepdims=True)) + 1e-06)
    normed = (stream * scale * norm_gain).astype(jnp.bfloat16)
    flat_routes = routes.reshape(-1)
    per_expert = TOKENS * 2 // EXPERTS
    hid_shard = HID // N_TP

    def one_expert(carry, expert):
        picked = jnp.nonzero(flat_routes == expert, size=per_expert)[0].astype(jnp.int32)
        rows = normed[picked // 2]
        gate_all = w_gate[expert]
        up_all = w_up[expert]
        down_all = w_down[expert]
        total = jnp.zeros((per_expert, D), jnp.float32)
        for shard in range(N_TP):
            low = shard * hid_shard
            gate = jnp.dot(rows, gate_all[:, low:low + hid_shard], preferred_element_type=jnp.float32)
            upper = jnp.dot(rows, up_all[:, low:low + hid_shard], preferred_element_type=jnp.float32)
            hidden = (jax.nn.silu(gate) * upper).astype(jnp.bfloat16)
            part = jnp.dot(hidden, down_all[low:low + hid_shard], preferred_element_type=jnp.float32).astype(jnp.bfloat16)
            part = lax.optimization_barrier(part)
            total = total + part.astype(jnp.float32)
        carry = carry.at[picked].set(total.astype(jnp.bfloat16))
        return (carry, None)
    start = jnp.zeros((TOKENS * 2, D), jnp.bfloat16)
    outputs, _ = lax.scan(one_expert, start, jnp.arange(EXPERTS, dtype=jnp.int32))
    expert_out = outputs.reshape(TOKENS, 2, D).astype(jnp.float32)
    weighted = lax.optimization_barrier(jnp.sum(route_weight[:, :, None] * expert_out, axis=1))
    return (stream + weighted).astype(jnp.bfloat16)
```

```python
import functools

import jax
import jax.numpy as jnp
from jax import lax
from jax.experimental import pallas as pl
from jax.experimental.pallas import tpu as pltpu
from jax.sharding import PartitionSpec as P

MESH = pl.DeviceIdType.MESH
BF16 = jnp.bfloat16
F32 = jnp.float32


def kernel(
    seq_ranks,
    tp_ranks,
    conv_hbm,
    pre_hbm,
    post_hbm,
    taps_ref,
    proj_hbm,
    resid_hbm,
    gain_ref,
    routes_ref,
    weight_ref,
    gate_hbm,
    up_hbm,
    down_hbm,
    out_ref,
    conv_in,
    pre_in,
    post_in,
    proj_w,
    resid_in,
    gate_w,
    up_w,
    down_w,
    halo,
    mixed,
    mixbuf,
    stream,
    normed,
    routes_all,
    weight_all,
    spread,
    rows,
    gathered,
    partial,
    half_a,
    half_b,
    from_left,
    from_right,
    returning,
    results,
    share_out,
    share_in,
    load_sem,
    misc_send,
    misc_recv,
    mix_send,
    mix_recv,
    out_send,
    out_recv,
    x_send,
    x_recv,
    back_send,
    back_recv,
):
    chips = seq_ranks // 2
    chunks = chips // 2
    sp = lax.axis_index("sp")
    tp = lax.axis_index("tp")
    z = sp // 2
    core = sp % 2
    tokens = out_ref.shape[0]
    width = out_ref.shape[1]
    channels = conv_in.shape[1]
    half = width // 2

    def chip(delta):
        return {"sp": lax.rem(z + delta + chips, chips) * 2 + core}

    def side(delta):
        return {"tp": lax.rem(tp + delta + tp_ranks, tp_ranks)}

    partner = {"sp": z * 2 + 1 - core}
    after = {"sp": lax.rem(sp + 1, seq_ranks)}
    before = {"sp": lax.rem(sp + seq_ranks - 1, seq_ranks)}

    loads = []
    for i, (src, dst) in enumerate(
        (
            (conv_hbm, conv_in),
            (pre_hbm, pre_in),
            (post_hbm, post_in),
            (resid_hbm, resid_in),
            (proj_hbm, proj_w),
            (gate_hbm, gate_w),
            (up_hbm, up_w),
            (down_hbm, down_w),
        )
    ):
        loads.append(pltpu.make_async_copy(src, dst, load_sem.at[i]))
        loads[-1].start()

    barrier = pltpu.get_barrier_semaphore()
    greeted = [after, before, partner]
    greeted += [side(d) for d in range(1, tp_ranks)]
    greeted += [chip(d) for d in range(1, chips)]
    for who in greeted:
        pl.semaphore_signal(barrier, inc=1, device_id=who, device_id_type=MESH)

    for load in loads[:3]:
        load.wait()

    taps = [
        taps_ref[k : k + 1, pl.ds(pl.multiple_of(tp * channels, channels), channels)]
        for k in range(3)
    ]

    def mix(gated, start):
        conv = gated[2:] * taps[2] + gated[1:-1] * taps[1] + gated[:-2] * taps[0]
        return (post_in[pl.ds(start, tokens), :].astype(F32) * conv).astype(BF16)

    for b in range(1, tp_ranks):
        lo = b * tokens
        span = pl.ds(lo - 16, tokens + 16)
        gated = pre_in[span, :].astype(F32) * conv_in[span, :].astype(F32)
        mixed[b] = mix(gated[14:], lo)

    pl.semaphore_wait(barrier, len(greeted))

    def remote(src, dst, send, recv, who):
        return pltpu.make_async_remote_copy(
            src_ref=src,
            dst_ref=dst,
            send_sem=send,
            recv_sem=recv,
            device_id=who,
            device_id_type=MESH,
        )

    last = pl.ds(conv_in.shape[0] - 16, 16)
    halos = [
        remote(conv_in.at[last, :], halo.at[0], misc_send.at[0], misc_recv.at[0], after),
        remote(pre_in.at[last, :], halo.at[1], misc_send.at[1], misc_recv.at[1], after),
    ]
    swaps = [
        remote(routes_ref, routes_all.at[1], misc_send.at[2], misc_recv.at[2], partner),
        remote(weight_ref, weight_all.at[1], misc_send.at[3], misc_recv.at[3], partner),
    ]
    for copy in halos:
        copy.start()
    for copy in swaps:
        copy.start()

    def mix_copy(d):
        return remote(
            mixed.at[lax.rem(tp + d, tp_ranks)],
            mixbuf.at[tp],
            mix_send.at[d],
            mix_recv.at[d],
            side(d),
        )

    for d in range(1, tp_ranks):

        @pl.when(lax.rem(tp + d, tp_ranks) != 0)
        def _():
            mix_copy(d).start()

    for copy in halos:
        copy.wait_recv()
    first = sp == 0
    halo_gated = halo[1].astype(F32) * halo[0].astype(F32)
    halo_gated = jnp.where(first, 0.0, halo_gated)
    head = pre_in[0:tokens, :].astype(F32) * conv_in[0:tokens, :].astype(F32)
    gated = jnp.concatenate([halo_gated[14:], head], axis=0)
    mixed[0] = mix(gated, 0)
    for d in range(1, tp_ranks):

        @pl.when(lax.rem(tp + d, tp_ranks) == 0)
        def _():
            mix_copy(d).start()

    mixbuf[tp] = mixed[tp]

    routes_all[0] = routes_ref[...]
    weight_all[0] = weight_ref[...]
    for copy in swaps:
        copy.wait_recv()
    slots = rows.shape[0] * rows.shape[1]
    experts = 2 * seq_ranks
    lane_e = lax.broadcasted_iota(jnp.int32, (2 * tokens, experts), 1)
    tri_r = lax.broadcasted_iota(jnp.int32, (2 * tokens, 2 * tokens), 0)
    tri_c = lax.broadcasted_iota(jnp.int32, (2 * tokens, 2 * tokens), 1)
    tri = (tri_c < tri_r).astype(BF16)
    lane_s = lax.broadcasted_iota(jnp.int32, (tokens, slots), 1)
    for who in range(2):
        owner = core if who == 0 else 1 - core
        flat = jnp.concatenate(
            [routes_all[who, :, 0:1], routes_all[who, :, 1:2]], axis=0
        )
        hot = (flat == lane_e).astype(F32)
        seen = jnp.dot(tri, hot.astype(BF16), preferred_element_type=F32)
        rank = jnp.sum(seen * hot, axis=1, keepdims=True).astype(jnp.int32)
        place = (flat // 4) * 16 + owner * 8 + (flat % 2) * 4 + rank
        place = jnp.where((flat // 2) % 2 == core, place, -1)
        w0 = weight_all[who, :, 0:1]
        w1 = weight_all[who, :, 1:2]
        hit0 = place[:tokens] == lane_s
        hit1 = place[tokens:] == lane_s
        zero = jnp.zeros((tokens, slots), F32)
        full = jnp.where(hit0, w0, zero) + jnp.where(hit1, w1, zero)
        high = full.astype(BF16)
        spread[0, who] = (hit0.astype(F32) + hit1.astype(F32)).astype(BF16)
        spread[1, who] = high
        spread[2, who] = (full - high.astype(F32)).astype(BF16)

    loads[3].wait()
    loads[4].wait()

    stream[...] = resid_in[...].astype(F32)
    for d in range(tp_ranks):
        src = lax.rem(tp - d + tp_ranks, tp_ranks)
        if d:
            mix_copy(d).wait_recv()
        cut = pl.ds(pl.multiple_of(src * channels, channels), channels)
        stream[...] += jnp.dot(
            mixbuf[src], proj_w[cut, :], preferred_element_type=F32
        )
    value = stream[...]
    scale = lax.rsqrt(jnp.mean(value * value, axis=-1, keepdims=True) + 1e-06)
    normed[0] = (value * scale * gain_ref[...]).astype(BF16)
    swap = remote(normed.at[0], normed.at[1], misc_send.at[4], misc_recv.at[4], partner)
    swap.start()
    contract = (((0,), (0,)), ((), ()))
    mine = lax.dot_general(
        spread[0, 0], normed[0], contract, preferred_element_type=F32
    )
    swap.wait_recv()
    both = mine + lax.dot_general(
        spread[0, 1], normed[1], contract, preferred_element_type=F32
    )
    rows[...] = both.astype(BF16).reshape(rows.shape)

    def deltas(k):
        up = k + 1
        down = chips - 1 - k
        return up, down

    def out_copy(k, which):
        delta = deltas(k)[which]
        slot = 2 * k + which
        to = lax.rem(z + delta, chips)
        return remote(
            rows.at[to],
            gathered.at[0, slot],
            out_send.at[slot],
            out_recv.at[slot],
            {"sp": to * 2 + core},
        )

    for k in range(chunks):
        out_copy(k, 0).start()
        if k < chunks - 1:
            out_copy(k, 1).start()
    gathered[0, chips - 1] = rows[z]

    def x_copy(stage, which, k):
        cut = pl.ds(2 * k, 2)
        low, high = pl.ds(0, half), pl.ds(half, half)
        if stage == 0:
            src = gathered.at[0, cut]
            dst = gathered.at[1 if which == 0 else 3, cut]
        elif stage == 1:
            part = low if which == 0 else high
            src = gathered.at[1 if which == 0 else 3, cut, :, part]
            dst = gathered.at[2, cut, :, part]
        elif stage == 2:
            src = partial.at[2, cut, :, low if which == 0 else high]
            dst = (half_a if which == 0 else half_b).at[cut]
        else:
            src = partial.at[3 if which == 0 else 1, cut]
            dst = (from_left if which == 0 else from_right).at[cut]
        return remote(
            src,
            dst,
            x_send.at[k, stage * 2 + which],
            x_recv.at[k, stage * 2 + which],
            side(1 if which == 0 else -1),
        )

    def back_copy(k, which):
        delta = deltas(k)[which]
        slot = 2 * k + which
        to = lax.rem(z - delta + chips, chips)
        return remote(
            returning.at[slot],
            results.at[z],
            back_send.at[slot],
            back_recv.at[slot],
            {"sp": to * 2 + core},
        )

    count = tp_ranks * 2 * rows.shape[1]
    line = lax.broadcasted_iota(jnp.int32, (count, channels), 0) % 8

    def arrive(k):
        out_copy(k, 0).wait_recv()

        @pl.when(k < chunks - 1)
        def _():
            out_copy(k, 1).wait_recv()

        x_copy(0, 0, k).start()
        x_copy(0, 1, k).start()

    def forward(k):
        for which in range(2):
            x_copy(0, which, k).wait_recv()
            x_copy(1, which, k).start()

    def compute(k):
        x_copy(1, 0, k).wait_recv()
        x_copy(1, 1, k).wait_recv()
        cut = pl.ds(2 * k, 2)
        block = gathered[:, cut].reshape(count, width)
        total = None
        for e in range(2):
            gate = jnp.dot(block, gate_w[e], preferred_element_type=F32)
            upper = jnp.dot(block, up_w[e], preferred_element_type=F32)
            hidden = jax.nn.silu(gate) * upper
            hidden = jnp.where(line < 4 if e == 0 else line >= 4, hidden, 0.0).astype(BF16)
            part = jnp.dot(hidden, down_w[e], preferred_element_type=F32)
            total = part if total is None else total + part
        partial[:, cut] = total.astype(BF16).reshape(tp_ranks, 2, rows.shape[1], width)
        x_copy(2, 0, k).start()
        x_copy(2, 1, k).start()

    def reduce(k):
        cut = pl.ds(2 * k, 2)
        for which in range(2):
            part = pl.ds(0 if which == 0 else half, half)
            own = 3 if which == 0 else 1
            got = half_a if which == 0 else half_b
            x_copy(2, which, k).wait_recv()
            partial[own, cut, :, part] = (
                partial[own, cut, :, part].astype(F32) + got[cut].astype(F32)
            ).astype(BF16)
            x_copy(3, which, k).start()

    def send_back(k):
        cut = pl.ds(2 * k, 2)
        x_copy(3, 0, k).wait_recv()
        x_copy(3, 1, k).wait_recv()
        returning[cut] = (
            partial[0, cut].astype(F32)
            + from_left[cut].astype(F32)
            + from_right[cut].astype(F32)
        ).astype(BF16)
        back_copy(k, 0).start()

        @pl.when(k < chunks - 1)
        def _():
            back_copy(k, 1).start()

    for load in loads[5:]:
        load.wait()

    stages = (forward, compute, reduce, send_back)

    def step(i, carry):
        for lag, work in enumerate(stages):
            k = i - 1 - lag

            @pl.when((k >= 0) & (k < chunks))
            def _():
                work(k)

        @pl.when(i < chunks)
        def _():
            arrive(i)

        return carry

    lax.fori_loop(0, chunks + len(stages), step, 0)

    results[z] = returning[chips - 1]
    for k in range(chunks):
        back_copy(k, 0).wait_recv()
        if k < chunks - 1:
            back_copy(k, 1).wait_recv()
    all_rows = results[...].reshape(slots, width)
    other = jnp.dot(spread[1, 1], all_rows, preferred_element_type=F32) + jnp.dot(
        spread[2, 1], all_rows, preferred_element_type=F32
    )
    share_out[...] = other.astype(BF16)
    share = remote(share_out, share_in, misc_send.at[5], misc_recv.at[5], partner)
    share.start()
    own = jnp.dot(spread[1, 0], all_rows, preferred_element_type=F32) + jnp.dot(
        spread[2, 0], all_rows, preferred_element_type=F32
    )
    stream[...] += own
    share.wait_recv()
    out_ref[...] = (stream[...] + share_in[...].astype(F32)).astype(BF16)

    for copy in halos + swaps + [swap, share]:
        copy.wait_send()
    for d in range(1, tp_ranks):
        mix_copy(d).wait_send()
    for k in range(chunks):
        for which in range(2 if k < chunks - 1 else 1):
            out_copy(k, which).wait_send()
            back_copy(k, which).wait_send()
        for stage in range(4):
            for which in range(2):
                x_copy(stage, which, k).wait_send()


def on_device(
    conv_input,
    pre_gate,
    post_gate,
    conv_taps,
    out_proj,
    residual_in,
    norm_gain,
    routes,
    route_weight,
    w_gate,
    w_up,
    w_down,
):
    tp_ranks = lax.axis_size("tp")
    seq_ranks = lax.axis_size("sp")
    chips = seq_ranks // 2
    tokens, width = residual_in.shape
    channels = conv_input.shape[1]
    hid = w_gate.shape[2]
    vmem = pl.BlockSpec(memory_space=pltpu.VMEM)
    hbm = pl.BlockSpec(memory_space=pl.ANY)
    dma = pltpu.SemaphoreType.DMA
    rows = (chips, 16, width)
    return pl.pallas_call(
        functools.partial(kernel, seq_ranks, tp_ranks),
        out_shape=jax.ShapeDtypeStruct((tokens, width), BF16),
        in_specs=[hbm, hbm, hbm, vmem, hbm, hbm, vmem, vmem, vmem, hbm, hbm, hbm],
        out_specs=vmem,
        scratch_shapes=[
            pltpu.VMEM(conv_input.shape, BF16),
            pltpu.VMEM(pre_gate.shape, BF16),
            pltpu.VMEM(post_gate.shape, BF16),
            pltpu.VMEM(out_proj.shape, BF16),
            pltpu.VMEM(residual_in.shape, BF16),
            pltpu.VMEM(w_gate.shape, BF16),
            pltpu.VMEM(w_up.shape, BF16),
            pltpu.VMEM(w_down.shape, BF16),
            pltpu.VMEM((2, 16, channels), BF16),
            pltpu.VMEM((tp_ranks, tokens, channels), BF16),
            pltpu.VMEM((tp_ranks, tokens, channels), BF16),
            pltpu.VMEM((tokens, width), F32),
            pltpu.VMEM((2, tokens, width), BF16),
            pltpu.VMEM((2, tokens, 2), jnp.int32),
            pltpu.VMEM((2, tokens, 2), F32),
            pltpu.VMEM((3, 2, tokens, chips * 16), BF16),
            pltpu.VMEM(rows, BF16),
            pltpu.VMEM((tp_ranks, *rows), BF16),
            pltpu.VMEM((tp_ranks, *rows), BF16),
            pltpu.VMEM((chips, 16, width // 2), BF16),
            pltpu.VMEM((chips, 16, width // 2), BF16),
            pltpu.VMEM(rows, BF16),
            pltpu.VMEM(rows, BF16),
            pltpu.VMEM(rows, BF16),
            pltpu.VMEM(rows, BF16),
            pltpu.VMEM((tokens, width), BF16),
            pltpu.VMEM((tokens, width), BF16),
            dma((8,)),
            dma((6,)),
            dma((6,)),
            dma((tp_ranks,)),
            dma((tp_ranks,)),
            dma((chips,)),
            dma((chips,)),
            dma((chips // 2, 8)),
            dma((chips // 2, 8)),
            dma((chips,)),
            dma((chips,)),
        ],
        compiler_params=pltpu.CompilerParams(
            collective_id=0,
            has_side_effects=True,
            vmem_limit_bytes=56 * 2**20,
        ),
        name="layer",
    )(
        conv_input,
        pre_gate,
        post_gate,
        conv_taps,
        out_proj,
        residual_in,
        norm_gain.reshape(1, width),
        routes,
        route_weight,
        w_gate,
        w_up,
        w_down,
    )


def solution(mesh):
    return jax.shard_map(
        on_device,
        mesh=mesh,
        in_specs=(
            P(("grp", "sp"), "tp"),
            P(("grp", "sp"), "tp"),
            P(("grp", "sp"), "tp"),
            P(),
            P(),
            P(("grp", "sp", "tp"), None),
            P(),
            P(("grp", "sp", "tp"), None),
            P(("grp", "sp", "tp"), None),
            P("sp", None, "tp"),
            P("sp", None, "tp"),
            P("sp", "tp", None),
        ),
        out_specs=P(("grp", "sp", "tp"), None),
        check_vma=False,
    )
```
